128 devices in a mesh: ep: 64 (over z, y, x), tp: 2 (over core).
Axes of the slice: x: 4, y: 4, z: 4, core: 2. Of those that a mesh axis runs over, the one named last changes fastest.
Arguments:
- tokens: bfloat16 [2048, 1024], P(('ep', 'tp')), may hold values from -6 to 6
- lengths: int32 [2048], P(('ep', 'tp')), may hold values from 1 to 1024
- cache_latent: bfloat16 [2048, 1024, 256], P(('ep', 'tp')), may hold values from -700 to 700
- cache_rope: bfloat16 [2048, 32, 1024], P(('ep', 'tp')), may hold values from -6 to 6
- attn_gain: bfloat16 [1024], replicated, may hold values from 0.099609375 to 1.8984375
- w_dq: bfloat16 [1024, 512], replicated, may hold values from -0.1875 to 0.1875
- q_gain: bfloat16 [512], replicated, may hold values from 0.099609375 to 1.8984375
- w_q_nope: bfloat16 [512, 1024], replicated, may hold values from -0.25 to 0.25
- w_q_rope: bfloat16 [512, 512], replicated, may hold values from -0.25 to 0.25
- w_dkv: bfloat16 [1024, 256], replicated, may hold values from -0.1875 to 0.1875
- kv_gain: bfloat16 [256], replicated, may hold values from 0.099609375 to 1.8984375
- w_krope: bfloat16 [1024, 32], replicated, may hold values from -0.1875 to 0.1875
- w_uk: bfloat16 [256, 1024], replicated, may hold values from -0.75 to 0.75
- w_uv: bfloat16 [256, 1024], replicated, may hold values from -0.375 to 0.375
- w_o: bfloat16 [1024, 1024], replicated, may hold values from -0.1875 to 0.1875
- post_gain: bfloat16 [1024], replicated, may hold values from 0.099609375 to 1.8984375
- moe_gain: bfloat16 [1024], replicated, may hold values from 0.099609375 to 1.8984375
- routes: int32 [2048, 4], P(('ep', 'tp')), may hold values from 0 to 63, all different within a row; in each aligned block of 16 rows (0 to 15, 16 to 31, ...) at most 3 rows name the same one
- route_scores: float32 [2048, 4], P(('ep', 'tp')), may hold values from 0.05 to 1
- expert_gate: bfloat16 [64, 1024, 512], P('ep', None, 'tp'), may hold values from -0.1875 to 0.1875
- expert_up: bfloat16 [64, 1024, 512], P('ep', None, 'tp'), may hold values from -0.1875 to 0.1875
- expert_down: bfloat16 [64, 512, 1024], P('ep', 'tp'), may hold values from -0.25 to 0.25
- shared_gate: bfloat16 [1024, 512], replicated, may hold values from -0.1875 to 0.1875
- shared_up: bfloat16 [1024, 512], replicated, may hold values from -0.1875 to 0.1875
- shared_down: bfloat16 [512, 1024], replicated, may hold values from -0.25 to 0.25
- dense_vec: bfloat16 [1024], replicated, may hold values from -0.1875 to 0.1875
- dense_w_gate: bfloat16 [1024, 8192], P(None, ('ep', 'tp')), may hold values from -0.1875 to 0.1875
- dense_w_up: bfloat16 [1024, 8192], P(None, ('ep', 'tp')), may hold values from -0.1875 to 0.1875
- dense_w_down: bfloat16 [8192, 1024], P(('ep', 'tp')), may hold values from -0.25 to 0.25
- out_gain: bfloat16 [1024], replicated, may hold values from 0.099609375 to 1.8984375
Outputs:
- hidden_out: bfloat16 [2048, 1024], P(('ep', 'tp'))
- new_latent: bfloat16 [2048, 256], P(('ep', 'tp'))
The draws below stay inside these ranges and needn't reach their ends.
Inputs may be any that keep to these rules, and one draw needn't show every extreme that they name: `routes`: each row names 4 different experts. In the 16 rows of one device no expert is named more than 3 times, a bound that some block reaches in some devices' rows.
All inputs are finite; a program needn't handle non-finite values.
Results may differ from the reference program's by a relative error of at most 0.011.
The reference program's roundings to bfloat16 on the way count: a program that leaves them out, or rounds other values in their place, can miss the bound.
Values may be sent and summed in bfloat16 or wider, within the bound.
A program may use at most 128 MiB of HBM per device.

```python
import math
from functools import partial
import jax
import jax.numpy as jnp
import numpy as np
from jax import lax

D = 1024
HEADS = 16
QL = 512
KL = 256
NOPE = 64
ROPE = 32
VDIM = 64
EFF = 512
SFF = 512
DFF = 8192
TOP_K = 4
SEQ_DEV = 16
CACHE_LEN = 1024
EXPERTS = 64
CAP = 3
TOKENS = 2048
N_TP = 2


def draw_cache_latent(key, part):
    base = jnp.clip(jax.random.normal(key, (TOKENS, CACHE_LEN, KL), jnp.float32), -6.0, 6.0)
    return base.astype(jnp.bfloat16)


def with_ends(array, own_key, low, largest):
    index_at = [jax.random.randint(jax.random.fold_in(own_key, axis), (), 0, length) for axis, length in enumerate(array.shape)]
    longest = array.shape.index(max(array.shape))
    neighbour = index_at[:longest] + [(index_at[longest] + 1) % array.shape[longest]] + index_at[longest + 1:]
    return array.at[tuple(index_at)].set(low).at[tuple(neighbour)].set(largest)


def raised(drawn, own_key, source, target, shards_of, factor):
    def block_of(position):
        return (jnp.arange(drawn.shape[position]) // (drawn.shape[position] // shards_of)).reshape((-1,) + (1,) * (drawn.ndim - 1 - position))

    near = jax.random.permutation(own_key, shards_of)[block_of(target)]
    far = (block_of(target) + shards_of // 2) % shards_of
    return jnp.where((block_of(source) == near) | (block_of(source) == far), factor * drawn, drawn)


def block_scale(key, extent, cuts, low, largest):
    factor_of, own = 1.0, jax.random.fold_in(key, 6)
    for dim, shards_of in cuts:
        heights = jnp.exp(jax.random.uniform(jax.random.fold_in(own, dim), (shards_of,), jnp.float32, low / len(cuts), largest / len(cuts)))
        factor_of = factor_of * jnp.repeat(heights, extent[dim] // shards_of).reshape([-1 if axis == dim else 1 for axis in range(len(extent))])
    return factor_of


def routed_block(own_key, own, number, rows, number_of, top, bound, skew):
    order = jax.random.permutation(own_key, number_of)
    crowded, ordinary = shares(number_of, rows * top, bound, skew, True), shares(number_of, rows * top, bound, skew, False)
    places = jnp.arange(number_of)

    def named(sizes, offset_by):
        used = int((sizes > 0).sum())
        fixed = max(1, used // 4)
        moved = fixed + (places - fixed + offset_by * (used - fixed)) % max(1, number_of - fixed)
        return jnp.zeros((number_of,), jnp.int32).at[order[jnp.where(places < fixed, places, moved)]].set(jnp.asarray(sizes, jnp.int32))

    sizes = jnp.where(number % 4 == 0, named(crowded, number // 4), named(ordinary, number - number // 4 - 1))
    mixed = jax.random.permutation(jax.random.fold_in(own, 3), number_of)
    donor, receiver = mixed[0:number_of // 2 * 2:2], mixed[1:number_of // 2 * 2:2]
    slack = jnp.minimum(sizes[donor] - 1, bound - sizes[receiver]) // 2
    slack = jnp.where((donor == order[0]) | (receiver == order[0]) | (sizes[receiver] == 0), 0, jnp.maximum(slack, 0))
    moved = jax.random.randint(jax.random.fold_in(own, 4), (number_of // 2,), 0, 1 << 20) % (slack + 1)
    sizes = sizes.at[donor].add(-moved).at[receiver].add(moved)
    labels = jnp.searchsorted(jnp.cumsum(sizes), jnp.arange(rows * top), side="right").astype(jnp.int32)
    table = labels.reshape(top, rows).T
    table = table[jax.random.permutation(jax.random.fold_in(own, 1), rows)]
    offset_by = jax.random.randint(jax.random.fold_in(own, 2), (rows, 1), 0, top)
    return jnp.take_along_axis(table, (jnp.arange(top)[None, :] + offset_by) % top, axis=1)


def shares(count, total, bound, slope, full):
    portions = [(1 << 20) // math.isqrt(standing ** slope) + 1 for standing in range(1, count + 1)]
    largest = bound if full else min(bound, max(-(-total // count), total * portions[0] // sum(portions)))
    least = 1 if total - largest >= count - 1 else 0
    holding, spare = [largest] + [least] * (count - 1), total - largest - least * (count - 1)
    while spare > 0:
        free = [i for i in range(1, count) if holding[i] < largest] or [i for i in range(1, count) if holding[i] < bound]
        mass, budget = sum([portions[i] for i in free]), spare
        for i in free:
            more = min(bound - holding[i], max(1, budget * portions[i] // mass), spare)
            holding[i] = holding[i] + more
            spare = spare - more
    return np.array(holding)


def bell_draw(rng, dims, deviation, reach, shards=(), kind=jnp.bfloat16):
    level = block_scale(rng, dims, shards, -0.22, 0.18) if shards else 1.0
    array = jax.random.normal(rng, dims, jnp.float32) * deviation * level
    return jnp.minimum(jnp.maximum(array, -reach), reach).astype(kind)


def noise_with(rng, dims, deviation, reach, cuts, heavy, kind=jnp.bfloat16):
    array = deviation * jax.random.normal(rng, dims, jnp.float32)
    if cuts:
        array = array * block_scale(rng, dims, cuts, -0.22, 0.18)
    return jnp.clip(raised(array, jax.random.fold_in(rng, 3), *heavy), -reach, reach).astype(kind)


def setup_inputs(seed: int = 0) -> dict:
    key_list = jax.random.split(jax.random.key(seed), 31)
    tokens = bell_draw(key_list[0], (TOKENS, D), 1.0, 6.0, ((0, 128),))
    lengths = with_ends(jax.random.randint(key_list[1], (TOKENS,), 1, CACHE_LEN + 1), jax.random.fold_in(key_list[1], 1), 1, CACHE_LEN).astype(jnp.int32)
    cache_latent = draw_cache_latent(jax.random.fold_in(key_list[30], 71), 0)
    cache_rope = bell_draw(key_list[3], (TOKENS, ROPE, CACHE_LEN), 1.0, 6.0, ((0, 128),))
    attn_gain = jnp.clip(1.0 + 0.18 * jax.random.normal(key_list[4], (D,), jnp.float32), 0.099609375, 1.8984375).astype(jnp.bfloat16)
    w_dq = bell_draw(key_list[5], (D, QL), D ** -0.5, 0.1875)
    q_gain = jnp.clip(1.0 + 0.18 * jax.random.normal(key_list[6], (QL,), jnp.float32), 0.099609375, 1.8984375).astype(jnp.bfloat16)
    w_q_nope = bell_draw(key_list[7], (QL, HEADS * NOPE), QL ** -0.5, 0.25)
    w_q_rope = bell_draw(key_list[8], (QL, HEADS * ROPE), QL ** -0.5, 0.25)
    w_dkv = bell_draw(key_list[9], (D, KL), D ** -0.5, 0.1875)
    kv_gain = jnp.clip(1.0 + 0.18 * jax.random.normal(key_list[10], (KL,), jnp.float32), 0.099609375, 1.8984375).astype(jnp.bfloat16)
    w_krope = bell_draw(key_list[11], (D, ROPE), D ** -0.5, 0.1875)
    w_uk = bell_draw(key_list[12], (KL, HEADS * NOPE), NOPE ** -0.5, 0.75)
    w_uv = bell_draw(key_list[13], (KL, HEADS * VDIM), KL ** -0.5, 0.375)
    w_o = bell_draw(key_list[14], (HEADS * VDIM, D), (HEADS * VDIM) ** -0.5, 0.1875)
    post_gain = jnp.clip(1.0 + 0.18 * jax.random.normal(key_list[15], (D,), jnp.float32), 0.099609375, 1.8984375).astype(jnp.bfloat16)
    moe_gain = jnp.clip(1.0 + 0.18 * jax.random.normal(key_list[16], (D,), jnp.float32), 0.099609375, 1.8984375).astype(jnp.bfloat16)
    routes_keys = jax.random.split(jax.random.fold_in(key_list[17], 1), TOKENS // SEQ_DEV)
    routes_turns = jax.random.permutation(jax.random.fold_in(key_list[17], 3), TOKENS // SEQ_DEV)
    routes = jax.vmap(lambda own, number: routed_block(jax.random.fold_in(key_list[17], 2), own, number, SEQ_DEV, EXPERTS, TOP_K, CAP, 2))(routes_keys, routes_turns).reshape((TOKENS, TOP_K))
    route_scores = jnp.clip(jnp.exp(math.log(1.0) - 2.9957323 * jax.random.uniform(key_list[18], (TOKENS, TOP_K), jnp.float32) ** block_scale(key_list[18], (TOKENS, TOP_K), ((0, 128),), -0.2, 0.2)), 0.05, 1.0)
    expert_gate = bell_draw(key_list[19], (EXPERTS, D, EFF), D ** -0.5, 0.1875, ((0, 64), (2, 2)))
    expert_up = bell_draw(key_list[20], (EXPERTS, D, EFF), D ** -0.5, 0.1875, ((0, 64), (2, 2)))
    expert_down = bell_draw(key_list[21], (EXPERTS, EFF, D), EFF ** -0.5, 0.25, ((0, 64), (1, 2)))
    shared_gate = bell_draw(key_list[22], (D, SFF), D ** -0.5, 0.1875)
    shared_up = bell_draw(key_list[23], (D, SFF), D ** -0.5, 0.1875)
    shared_down = bell_draw(key_list[24], (SFF, D), SFF ** -0.5, 0.25)
    dense_vec = bell_draw(key_list[25], (D,), D ** -0.5, 0.1875)
    dense_w_gate = bell_draw(key_list[26], (D, DFF), D ** -0.5, 0.1875, ((1, 128),))
    dense_w_up = bell_draw(key_list[27], (D, DFF), D ** -0.5, 0.1875, ((1, 128),))
    dense_w_down = noise_with(key_list[28], (DFF, D), DFF ** -0.5, 0.25, ((0, 128),), (0, 1, 128, 5.5))
    out_gain = jnp.clip(1.0 + 0.18 * jax.random.normal(key_list[29], (D,), jnp.float32), 0.099609375, 1.8984375).astype(jnp.bfloat16)
    return dict(tokens=tokens, lengths=lengths, cache_latent=cache_latent, cache_rope=cache_rope, attn_gain=attn_gain, w_dq=w_dq, q_gain=q_gain, w_q_nope=w_q_nope, w_q_rope=w_q_rope, w_dkv=w_dkv, kv_gain=kv_gain, w_krope=w_krope, w_uk=w_uk, w_uv=w_uv, w_o=w_o, post_gain=post_gain, moe_gain=moe_gain, routes=routes, route_scores=route_scores, expert_gate=expert_gate, expert_up=expert_up, expert_down=expert_down, shared_gate=shared_gate, shared_up=shared_up, shared_down=shared_down, dense_vec=dense_vec, dense_w_gate=dense_w_gate, dense_w_up=dense_w_up, dense_w_down=dense_w_down, out_gain=out_gain)


eps = 1e-06
rope_base = 10000.0
routed_scale = 2.5

def rms_scale(value, gain):
    value = value.astype(jnp.float32)
    inverse = lax.rsqrt(lax.optimization_barrier(jnp.mean(value * value, axis=-1, keepdims=True)) + eps)
    return value * inverse * gain.astype(jnp.float32)

def angles(lengths):
    half = ROPE // 2
    freqs = rope_base ** (-jnp.arange(half, dtype=jnp.float32) / half)
    angle = lengths.astype(jnp.float32)[:, None] * freqs[None, :]
    return (jnp.cos(angle), jnp.sin(angle))

def rotate(value, cosine, sine):
    half = value.shape[-1] // 2
    first, second = (value[..., :half], value[..., half:])
    return jnp.concatenate([first * cosine - second * sine, second * cosine + first * sine], axis=-1)

def slot_table(ids, scores, experts, cap):
    rows, top = ids.shape
    norm = scores / lax.optimization_barrier(jnp.sum(scores, axis=1, keepdims=True)) * routed_scale
    flat = ids.reshape(-1)
    onehot = (flat[:, None] == jnp.arange(experts, dtype=jnp.int32)[None, :]).astype(jnp.int32)
    rank = jnp.cumsum(onehot, axis=0) - 1
    hit = onehot[:, :, None] * (rank[:, :, None] == jnp.arange(cap, dtype=jnp.int32)[None, None, :]).astype(jnp.int32)
    owner = jnp.arange(rows * top, dtype=jnp.int32) // top
    token_of = lax.optimization_barrier(jnp.sum(hit * owner[:, None, None], axis=0)).astype(jnp.int32)
    weight_of = lax.optimization_barrier(jnp.sum(hit.astype(norm.dtype) * norm.reshape(-1)[:, None, None], axis=0))
    return (token_of, weight_of)

def attend_block(block, weights):
    tokens, lengths, latent, rope_keys = block
    attn_gain, w_dq, q_gain, w_q_nope, w_q_rope, w_dkv, kv_gain, w_krope, w_uk, w_uv, w_o, post_gain = weights
    f32 = jnp.float32
    bf16 = jnp.bfloat16
    seqs = tokens.shape[0]
    normed = rms_scale(tokens, attn_gain).astype(bf16)
    q_normed = rms_scale(jnp.dot(normed, w_dq, preferred_element_type=f32), q_gain).astype(bf16)
    q_nope = jnp.dot(q_normed, w_q_nope, preferred_element_type=f32).astype(bf16).reshape(seqs, HEADS, NOPE)
    cosine, sine = angles(lengths)
    q_raw = jnp.dot(q_normed, w_q_rope, preferred_element_type=f32).reshape(seqs, HEADS, ROPE)
    q_rot = rotate(q_raw, cosine[:, None, :], sine[:, None, :]).astype(bf16)
    new_latent = rms_scale(jnp.dot(normed, w_dkv, preferred_element_type=f32), kv_gain).astype(bf16)
    new_rope = rotate(jnp.dot(normed, w_krope, preferred_element_type=f32), cosine, sine).astype(bf16)
    query_lat = jnp.einsum('shn,chn->shc', q_nope.astype(f32), w_uk.reshape(KL, HEADS, NOPE).astype(f32)).astype(bf16)
    scale = (NOPE + ROPE) ** (-0.5)
    past = jnp.einsum('shc,slc->shl', query_lat.astype(f32), latent.astype(f32))
    past = (past + jnp.einsum('shr,srl->shl', q_rot.astype(f32), rope_keys.astype(f32))) * scale
    own = jnp.einsum('shc,sc->sh', query_lat.astype(f32), new_latent.astype(f32))
    own = (own + jnp.einsum('shr,sr->sh', q_rot.astype(f32), new_rope.astype(f32))) * scale
    valid = jnp.arange(CACHE_LEN, dtype=jnp.int32)[None, None, :] < lengths[:, None, None]
    top = jnp.maximum(lax.optimization_barrier(jnp.max(jnp.where(valid, past, -1e+30), axis=-1)), own)
    past_weight = jnp.where(valid, jnp.exp(past - top[..., None]), 0.0)
    own_weight = jnp.exp(own - top)
    total = lax.optimization_barrier(jnp.sum(past_weight, axis=-1)) + own_weight
    past_prob = (past_weight / total[..., None]).astype(bf16)
    own_prob = (own_weight / total).astype(bf16)
    mixed = jnp.einsum('shl,slc->shc', past_prob.astype(f32), latent.astype(f32))
    mixed = (mixed + own_prob.astype(f32)[..., None] * new_latent.astype(f32)[:, None, :]).astype(bf16)
    head_out = jnp.einsum('shc,chv->shv', mixed.astype(f32), w_uv.reshape(KL, HEADS, VDIM).astype(f32)).astype(bf16)
    attn_out = jnp.dot(head_out.reshape(seqs, HEADS * VDIM), w_o, preferred_element_type=f32)
    first = (tokens.astype(f32) + rms_scale(attn_out, post_gain)).astype(bf16)
    return (first, new_latent)

def reference(tokens, lengths, cache_latent, cache_rope, attn_gain, w_dq, q_gain, w_q_nope, w_q_rope, w_dkv, kv_gain, w_krope, w_uk, w_uv, w_o, post_gain, moe_gain, routes, route_scores, expert_gate, expert_up, expert_down, shared_gate, shared_up, shared_down, dense_vec, dense_w_gate, dense_w_up, dense_w_down, out_gain):
    f32 = jnp.float32
    bf16 = jnp.bfloat16
    groups = TOKENS // SEQ_DEV
    weights = (attn_gain, w_dq, q_gain, w_q_nope, w_q_rope, w_dkv, kv_gain, w_krope, w_uk, w_uv, w_o, post_gain)
    blocks = (tokens.reshape(groups, SEQ_DEV, D), lengths.reshape(groups, SEQ_DEV), cache_latent.reshape(groups, SEQ_DEV, CACHE_LEN, KL), cache_rope.reshape(groups, SEQ_DEV, ROPE, CACHE_LEN))
    first, new_latent = lax.map(partial(attend_block, weights=weights), blocks)
    first = first.reshape(TOKENS, D)
    new_latent = new_latent.reshape(TOKENS, KL)
    moe_in = rms_scale(first, moe_gain).astype(bf16)
    shared_act = (jax.nn.silu(jnp.dot(moe_in, shared_gate, preferred_element_type=f32)) * jnp.dot(moe_in, shared_up, preferred_element_type=f32)).astype(bf16)
    shared_out = jnp.dot(shared_act, shared_down, preferred_element_type=f32)
    dense_act = (jax.nn.silu(jnp.dot(moe_in, dense_w_gate, preferred_element_type=f32)) * jnp.dot(moe_in, dense_w_up, preferred_element_type=f32)).astype(bf16)
    dense_out = jnp.dot(dense_act, dense_w_down, preferred_element_type=f32)
    gate = jax.nn.sigmoid(jnp.dot(moe_in, dense_vec, preferred_element_type=f32))
    token_all, weight_all = jax.vmap(partial(slot_table, experts=EXPERTS, cap=CAP))(routes.reshape(groups, SEQ_DEV, TOP_K), route_scores.reshape(groups, SEQ_DEV, TOP_K))
    base = (jnp.arange(groups, dtype=jnp.int32) * SEQ_DEV)[:, None]

    def expert_step(routed, expert):
        where_rows = (lax.dynamic_index_in_dim(token_all, expert, 1, keepdims=False) + base).reshape(-1).astype(jnp.int32)
        weight = lax.dynamic_index_in_dim(weight_all, expert, 1, keepdims=False).reshape(-1)
        rows = moe_in[where_rows]
        hidden_gate = jnp.dot(rows, expert_gate[expert], preferred_element_type=f32)
        hidden_up = jnp.dot(rows, expert_up[expert], preferred_element_type=f32)
        act = (jax.nn.silu(hidden_gate) * hidden_up).astype(bf16)
        act_parts = act.astype(f32).reshape(-1, N_TP, EFF // N_TP)
        down_parts = expert_down[expert].astype(f32).reshape(N_TP, EFF // N_TP, D)
        parts = jnp.einsum('rtf,tfd->rtd', act_parts, down_parts).astype(bf16).astype(f32)
        out = lax.optimization_barrier(jnp.sum(parts, axis=1))
        return (routed.at[where_rows].add(out * weight[:, None].astype(f32)), None)
    routed, _ = lax.scan(expert_step, jnp.zeros((TOKENS, D), f32), jnp.arange(EXPERTS, dtype=jnp.int32))
    mixture = routed + shared_out + gate[:, None] * dense_out
    hidden_out = (first.astype(f32) + rms_scale(mixture, out_gain)).astype(bf16)
    return (hidden_out, new_latent)
```

```python
import math

import jax
import jax.numpy as jnp
from jax import lax
from jax.experimental import pallas as pl
from jax.experimental.pallas import tpu as pltpu
from jax.sharding import PartitionSpec as P

f32 = jnp.float32
bf16 = jnp.bfloat16
EPS = 1e-6
NT = (((1,), (1,)), ((), ()))
NN = (((1,), (0,)), ((), ()))
TN = (((0,), (0,)), ((), ()))
MESH = pl.DeviceIdType.MESH

S, H, NOPE, ROPE, L, C, D = 16, 16, 64, 32, 1024, 256, 1024
SCALE = (NOPE + ROPE) ** -0.5
CHIPS, PLANE = 64, 16
SLOTS, QB = 4, 4
PIECE = SLOTS * QB


def dot(a, b, dims=NN):
    return lax.dot_general(a, b, dims, preferred_element_type=f32)


def iota(shape, dim):
    return lax.broadcasted_iota(jnp.int32, shape, dim)


def row_of(ref):
    blocks = ref[...].astype(f32)
    return jnp.concatenate([blocks[r : r + 1, :] for r in range(blocks.shape[0])], axis=1)


def rms(value, gain):
    inverse = lax.rsqrt(jnp.mean(value * value, axis=-1, keepdims=True) + EPS)
    return value * inverse * gain


def silu(v):
    return v / (1.0 + jnp.exp(-v))


def rope_tables(len_ref):
    half = ROPE // 2
    lane = iota((S, 128), 1) % half
    row = iota((S, 128), 0)
    pos = jnp.zeros((S, 128), jnp.int32)
    for s in range(S):
        pos = jnp.where(row == s, len_ref[s], pos)
    freq = jnp.exp(lane.astype(f32) * (-math.log(10000.0) / half))
    angle = pos.astype(f32) * freq
    return jnp.cos(angle), jnp.sin(angle)


def rotate128(value, cosine, sine):
    half = ROPE // 2
    first = (iota(value.shape, 1) % ROPE) < half
    other = jnp.where(first, -pltpu.roll(value, 128 - half, 1), pltpu.roll(value, half, 1))
    return value * cosine + other * sine


def halves(value):
    high = value.astype(bf16)
    return high, (value - high.astype(f32)).astype(bf16)


def route_tables(routes, scores, pick, weigh):
    ids = routes[...].astype(bf16)
    spread = (iota((S, QB * S), 1) % S == iota((S, QB * S), 0)).astype(bf16)
    named = dot(ids, spread)
    expert = iota((CHIPS, QB * S), 0).astype(f32)
    count = jnp.zeros((CHIPS, QB * S), f32)
    for k in range(4):
        count += jnp.where(named[k : k + 1, :] == expert, 1.0, 0.0)
    r, c = iota((QB * S, QB * S), 0), iota((QB * S, QB * S), 1)
    before = ((r < S) & (r < c % S)).astype(bf16)
    rank = dot(count.astype(bf16), before)
    at = jnp.where(count > 0.5, rank, -1.0)
    shape = (CHIPS, PIECE, QB * S)
    i, n = iota(shape, 1), iota(shape, 2)
    here = (at[:, None, :] == (i % SLOTS).astype(f32)) & (i // SLOTS == n // S)
    pick[...] = jnp.where(here, 1.0, 0.0).reshape(CHIPS * PIECE, QB * S).astype(bf16)

    norm = scores[...]
    norm = norm / jnp.sum(norm, axis=0, keepdims=True) * 2.5
    high, low = halves(norm)
    select = (iota((QB * S, S), 0) % S == iota((QB * S, S), 1)).astype(bf16)
    named_t, high_t, low_t = dot(select, ids, NT), dot(select, high, NT), dot(select, low, NT)
    expert_t = iota((QB * S, CHIPS), 1).astype(f32)
    count_t = jnp.zeros((QB * S, CHIPS), f32)
    w_high, w_low = count_t, count_t
    for k in range(4):
        hit = named_t[:, k : k + 1] == expert_t
        count_t += jnp.where(hit, 1.0, 0.0)
        w_high += jnp.where(hit, high_t[:, k : k + 1], 0.0)
        w_low += jnp.where(hit, low_t[:, k : k + 1], 0.0)
    before_t = ((c < S) & (c < r % S)).astype(bf16)
    rank_t = dot(before_t, count_t.astype(bf16))
    widen = (iota((CHIPS, CHIPS * PIECE), 1) // PIECE == iota((CHIPS, CHIPS * PIECE), 0)).astype(bf16)
    shape = (QB * S, CHIPS * PIECE)
    m = iota(shape, 1)
    here = (dot(rank_t.astype(bf16), widen) == (m % SLOTS).astype(f32)) & (
        (m // SLOTS) % QB == iota(shape, 0) // S
    )
    weigh[0 : QB * S, :] = jnp.where(here, dot(w_high.astype(bf16), widen), 0.0).astype(bf16)
    weigh[QB * S : 2 * QB * S, :] = jnp.where(here, dot(w_low.astype(bf16), widen), 0.0).astype(bf16)


def kernel(
    len_ref, tok_h, lat_h, rope_h, ag, wdq_h, qg, wqn_h, wqr_h, wdkv_h, kvg, wkr_h, wuk_h, wuv_h, wo_h, pg, mg,
    routes, scores, eg_h, eu_h, ed_h, sg_h, su_h, sd_h, dvec, dg_h, du_h, dd_h, og,
    out_o, lat_o,
    tok, lat, rope, wdq, wqn, wqr, wdkv, wkr, wuk, wuv, wo, ql, qr, own_s, mixed, nlat,
    eg, eu, ed, sg, su, sd, dg, du, dd, pick, weigh,
    moe, send, recv, back, home, rows, parts, sums,
    sems, lsem, esem, dsem, zsem_s, zsem_r, fsem_s, fsem_r, asem_s, asem_r, bsem_s, bsem_r, gsem_s, gsem_r, psem_s, psem_r,
):
    ep = lax.axis_index("ep")
    tp = lax.axis_index("tp")
    z, y, x = ep // 16, (ep // 4) % 4, ep % 4
    plane = ep % 16

    def remote(src, dst, s_sem, r_sem, chip, core):
        return pltpu.make_async_remote_copy(
            src_ref=src, dst_ref=dst, send_sem=s_sem, recv_sem=r_sem, device_id=(chip, core), device_id_type=MESH
        )

    early = [(tok_h, tok), (wdq_h, wdq), (wdkv_h, wdkv), (wkr_h, wkr), (wqn_h, wqn), (wqr_h, wqr), (wuk_h, wuk)]
    late = [(wuv_h, wuv), (wo_h, wo), (eg_h, eg.at[0:1]), (eu_h, eu.at[0:1]), (ed_h, ed.at[0:1]),
            (sg_h, sg), (su_h, su), (sd_h, sd), (dg_h, dg.at[0]), (du_h, du.at[0]), (dd_h, dd.at[0])]
    early = [pltpu.make_async_copy(a, b, sems.at[i]) for i, (a, b) in enumerate(early)]
    late = [pltpu.make_async_copy(a, b, sems.at[7 + i]) for i, (a, b) in enumerate(late)]

    def lat_cp(g):
        return (
            pltpu.make_async_copy(lat_h.at[pl.ds(4 * g, 4)], lat.at[pl.ds(4 * g, 4)], lsem.at[g, 0]),
            pltpu.make_async_copy(rope_h.at[pl.ds(4 * g, 4)], rope.at[pl.ds(4 * g, 4)], lsem.at[g, 1]),
        )

    for c in early:
        c.start()
    for g in range(4):
        for c in lat_cp(g):
            c.start()
    for c in late:
        c.start()

    barrier = pltpu.get_barrier_semaphore()

    def chip_of(k):
        kz, ky, kx = k // 16, (k // 4) % 4, k % 4
        return ((z + kz) % 4) * 16 + ((y + ky) % 4) * 4 + (x + kx) % 4

    def greet(k, _):
        pl.semaphore_signal(barrier, inc=1, device_id=(chip_of(k), tp), device_id_type=MESH)
        return 0

    lax.fori_loop(1, CHIPS, greet, 0)
    pl.semaphore_signal(barrier, inc=1, device_id=(ep, 1 - tp), device_id_type=MESH)

    route_tables(routes, scores, pick, weigh)

    cosine, sine = rope_tables(len_ref)
    early[0].wait()
    tokens = tok[...].astype(f32)
    normed = rms(tokens, row_of(ag)).astype(bf16)
    early[1].wait()
    qn = rms(dot(normed, wdq[...]), row_of(qg)).astype(bf16)
    early[2].wait()
    nl = rms(dot(normed, wdkv[...]), row_of(kvg)).astype(bf16)
    nlat[...] = nl.astype(f32)
    lat_o[...] = nl
    early[3].wait()
    kr = dot(normed, jnp.concatenate([wkr[...]] * 4, axis=0), NT)
    kr = rotate128(kr, cosine, sine).astype(bf16)
    early[4].wait()
    qnope = dot(qn, wqn[...]).astype(bf16).astype(f32)
    head = iota((H, D), 1) // NOPE == iota((H, D), 0)
    qm = jnp.where(head[None], qnope[:, None, :], 0.0).reshape(S * H, D).astype(bf16)
    early[5].wait()
    qraw = dot(qn, wqr[...])
    qrot = jnp.concatenate(
        [rotate128(qraw[:, 128 * i : 128 * i + 128], cosine, sine) for i in range(4)], axis=1
    )
    qrot = qrot.astype(bf16).astype(f32)
    headr = iota((H, H * ROPE), 1) // ROPE == iota((H, H * ROPE), 0)
    qrm = jnp.where(headr[None], qrot[:, None, :], 0.0).reshape(S * H, H * ROPE).astype(bf16)
    fold = (iota((H * ROPE, 128), 0) % ROPE == iota((H * ROPE, 128), 1)).astype(bf16)
    qrf = dot(qrm, fold)
    qr[...] = qrf.astype(bf16)
    early[6].wait()
    qlat = dot(qm, wuk[...], NT).astype(bf16)
    ql[...] = qlat
    own = jnp.sum(qlat.astype(f32).reshape(S, H, C) * nl.astype(f32)[:, None, :], axis=-1, keepdims=True)
    own += jnp.sum(qrf.reshape(S, H, 128) * kr.astype(f32)[:, None, :], axis=-1, keepdims=True)
    own_s[...] = own.reshape(S * H, 1) * SCALE

    pl.semaphore_wait(barrier, CHIPS)
    up_chip = ((z + 1) % 4) * 16 + plane
    down_chip = ((z + 3) % 4) * 16 + plane
    to_core = [
        remote(eg_h, eg.at[1:2], esem.at[0, 0], esem.at[1, 0], ep, 1 - tp),
        remote(eu_h, eu.at[1:2], esem.at[0, 1], esem.at[1, 1], ep, 1 - tp),
        remote(ed_h, ed.at[1:2], esem.at[0, 2], esem.at[1, 2], ep, 1 - tp),
        remote(dg_h, dg.at[4], esem.at[0, 3], esem.at[1, 3], ep, 1 - tp),
        remote(du_h, du.at[4], esem.at[0, 4], esem.at[1, 4], ep, 1 - tp),
        remote(dd_h, dd.at[4], esem.at[0, 5], esem.at[1, 5], ep, 1 - tp),
    ]
    to_chips = []
    for i, (h, buf) in enumerate([(dg_h, dg), (du_h, du), (dd_h, dd)]):
        to_chips.append(remote(h, buf.at[1], zsem_s.at[0, i], zsem_r.at[0, i], up_chip, tp))
        to_chips.append(remote(h, buf.at[3], zsem_s.at[1, i], zsem_r.at[1, i], down_chip, tp))
    for c in to_chips + to_core:
        c.start()

    lane = iota((H, L), 1)

    def group(g, _):
        for c in lat_cp(g):
            c.wait()
        base = pl.multiple_of(g * 4 * H, 4 * H)
        rows4 = pl.ds(base, 4 * H)
        sc = jnp.concatenate(
            [
                dot(ql[pl.ds(base + i * H, H)], lat[g * 4 + i], NT)
                + dot(qr[pl.ds(base + i * H, H), :][:, :ROPE], rope[g * 4 + i])
                for i in range(4)
            ],
            axis=0,
        )
        sc = sc * SCALE
        valid = jnp.concatenate([lane < len_ref[g * 4 + i] for i in range(4)], axis=0)
        ow = own_s[rows4]
        top = jnp.maximum(jnp.max(jnp.where(valid, sc, -1e30), axis=-1, keepdims=True), ow)
        w = jnp.where(valid, jnp.exp(sc - top), 0.0)
        ow = jnp.exp(ow - top)
        inv = 1.0 / (jnp.sum(w, axis=-1, keepdims=True) + ow)
        pb = (w * inv).astype(bf16)
        ob = (ow * inv).astype(bf16).astype(f32)
        for i in range(4):
            m = dot(pb[i * H : i * H + H], lat[g * 4 + i]) + ob[i * H : i * H + H] * nlat[pl.ds(g * 4 + i, 1)]
            mixed[pl.ds(base + i * H, H)] = m.astype(bf16)
        return 0

    lax.fori_loop(0, 4, group, 0)
    late[0].wait()
    full = dot(mixed[...], wuv[...]).reshape(S, H, D)
    ho = jnp.sum(jnp.where(head[None], full, 0.0), axis=1).astype(bf16)
    late[1].wait()
    first = (tokens + rms(dot(ho, wo[...]), row_of(pg))).astype(bf16)
    moe_in = rms(first.astype(f32), row_of(mg)).astype(bf16)
    moe[...] = moe_in

    blocks = jnp.concatenate([moe_in[:, 256 * q : 256 * q + 256] for q in range(QB)], axis=0)
    send[...] = dot(pick[...], blocks).astype(bf16).reshape(CHIPS, PIECE, 256)
    recv[ep] = send[ep]
    rows[plane] = moe_in

    def dispatch(k, _):
        chip = chip_of(k)
        remote(send.at[chip], recv.at[ep], asem_s, asem_r.at[k // 16], chip, tp).start()
        return 0

    def gather(k, _):
        chip = chip_of(k)
        remote(moe, rows.at[plane], gsem_s, gsem_r, chip, tp).start()
        return 0

    lax.fori_loop(1, CHIPS, dispatch, 0)
    lax.fori_loop(1, PLANE, gather, 0)

    for i, buf in enumerate([dg, du, dd]):
        remote(buf.at[1], buf.at[1], zsem_s.at[0, i], zsem_r.at[0, i], up_chip, tp).wait_recv()
        remote(buf.at[3], buf.at[3], zsem_s.at[1, i], zsem_r.at[1, i], down_chip, tp).wait_recv()
    onward = jnp.where(tp == 0, 1, 3)
    next_chip = jnp.where(tp == 0, up_chip, down_chip)
    onwards, crossing = [], []
    for i, buf in enumerate([dg, du, dd]):
        onwards.append(remote(buf.at[onward], buf.at[2], fsem_s.at[0, i], fsem_r.at[0, i], next_chip, tp))
    for i, buf in enumerate([dg, du, dd]):
        crossing.append(remote(buf.at[1], buf.at[5], fsem_s.at[1, i], fsem_r.at[1, i], ep, 1 - tp))
        crossing.append(remote(buf.at[3], buf.at[7], fsem_s.at[2, i], fsem_r.at[2, i], ep, 1 - tp))
    for c in onwards + crossing:
        c.start()

    for c in late[5:8]:
        c.wait()
    shared_act = (silu(dot(moe_in, sg[...])) * dot(moe_in, su[...])).astype(bf16)
    mixture = dot(shared_act, sd[...])

    for c in late[2:5]:
        c.wait()
    for c in to_core[0:3]:
        c.wait_recv()
    m, n = iota((256, 256), 0), iota((256, 256), 1)
    sort = ((m // 64 == (n // SLOTS) % QB) & ((m % 64) // SLOTS == n // PIECE) & (m % SLOTS == n % SLOTS))
    sort = jnp.where(sort, 1.0, 0.0).astype(bf16)
    for i in range(4):
        g = (z + 4 - i) % 4
        lo = pl.multiple_of(g * PLANE, PLANE)
        if i == 0:
            pltpu.make_async_copy(recv.at[0:15], recv.at[0:15], asem_r.at[0]).wait()
        else:
            pltpu.make_async_copy(recv.at[0:16], recv.at[0:16], asem_r.at[i]).wait()
        got = dot(sort, recv[pl.ds(lo, PLANE)].reshape(PLANE * PIECE, 256)).astype(bf16)
        rows_in = jnp.concatenate([got[64 * q : 64 * q + 64] for q in range(QB)], axis=1)
        total = jnp.zeros((64, D), f32)
        for part in range(2):
            act = (silu(dot(rows_in, eg[part])) * dot(rows_in, eu[part])).astype(bf16)
            total += dot(act, ed[part]).astype(bf16).astype(f32)
        total = total.astype(bf16)
        total = jnp.concatenate([total[:, 256 * q : 256 * q + 256] for q in range(QB)], axis=0)
        back[pl.ds(lo, PLANE)] = dot(sort, total, TN).astype(bf16).reshape(PLANE, PIECE, 256)
        if i == 0:
            home[ep] = back[ep]

        def give(k, _):
            chip = chip_of(((4 - i) % 4) * 16 + k)
            remote(back.at[chip], home.at[ep], bsem_s, bsem_r, chip, tp).start()
            return 0

        lax.fori_loop(1 if i == 0 else 0, PLANE, give, 0)

    for c in onwards:
        c.wait_recv()
    last = [
        remote(buf.at[2], buf.at[6], fsem_s.at[3, i], fsem_r.at[3, i], ep, 1 - tp) for i, buf in enumerate([dg, du, dd])
    ]
    for c in last:
        c.start()
    for c in late[8:11]:
        c.wait()
    for c in to_core[3:6] + crossing + last:
        c.wait_recv()
    pltpu.make_async_copy(rows.at[0:15], rows.at[0:15], gsem_r).wait()
    all_rows = rows[...].reshape(PLANE * S, D)
    gate_h = dot(all_rows, dg[...].reshape(512, D), NT)
    up_h = dot(all_rows, du[...].reshape(512, D), NT)
    act = (silu(gate_h) * up_h).astype(bf16)
    parts[...] = dot(act, dd[...].reshape(512, D)).astype(bf16).reshape(PLANE, S, D)
    sums[plane] = parts[plane]

    def share(k, _):
        chip = chip_of(k)
        remote(parts.at[chip % 16], sums.at[plane], psem_s, psem_r, chip, tp).start()
        return 0

    lax.fori_loop(1, PLANE, share, 0)

    gate = jnp.sum(moe_in.astype(f32) * row_of(dvec), axis=-1, keepdims=True)
    gate = 1.0 / (1.0 + jnp.exp(-gate))

    pltpu.make_async_copy(home.at[0:63], home.at[0:63], bsem_r).wait()
    routed = dot(weigh[...], home[...].reshape(CHIPS * PIECE, 256))
    routed = routed[0:64] + routed[64:128]
    mixture += jnp.concatenate([routed[S * q : S * q + S] for q in range(QB)], axis=1)

    pltpu.make_async_copy(sums.at[0:15], sums.at[0:15], psem_r).wait()
    dense = jnp.zeros((S, D), f32)
    for p in range(PLANE):
        dense += sums[p].astype(f32)
    mixture += gate * dense
    out_o[...] = (first.astype(f32) + rms(mixture, row_of(og))).astype(bf16)

    for c in to_chips + to_core + onwards + crossing + last:
        c.wait_send()
    pltpu.make_async_copy(send.at[0:63], send.at[0:63], asem_s).wait()
    pltpu.make_async_copy(back.at[0:63], back.at[0:63], bsem_s).wait()
    pltpu.make_async_copy(rows.at[0:15], rows.at[0:15], gsem_s).wait()
    pltpu.make_async_copy(parts.at[0:15], parts.at[0:15], psem_s).wait()


def step(
    tokens, lengths, latent, rope, ag, wdq, qg, wqn, wqr, wdkv, kvg, wkr, wuk, wuv, wo, pg, mg,
    routes, scores, eg, eu, ed, sg, su, sd, dvec, dg, du, dd, og,
):
    anyspec = pl.BlockSpec(memory_space=pl.ANY)
    vm = pl.BlockSpec(memory_space=pltpu.VMEM)
    smem = pl.BlockSpec(memory_space=pltpu.SMEM)

    def tile(v):
        return v.reshape(v.shape[0] // 128, 128)

    operands = [
        (lengths, smem), (tokens, anyspec), (latent, anyspec), (rope, anyspec), (tile(ag), vm), (wdq, anyspec), (tile(qg), vm),
        (wqn, anyspec), (wqr, anyspec), (wdkv, anyspec), (tile(kvg), vm), (wkr.T, anyspec), (wuk, anyspec), (wuv, anyspec),
        (wo, anyspec), (tile(pg), vm), (tile(mg), vm), (routes.T, vm), (scores.T, vm), (eg, anyspec), (eu, anyspec),
        (ed, anyspec), (sg, anyspec), (su, anyspec), (sd, anyspec), (tile(dvec), vm), (dg.T, anyspec), (du.T, anyspec),
        (dd, anyspec), (tile(og), vm),
    ]

    def v(*shape, dtype=bf16):
        return pltpu.VMEM(shape, dtype)

    dma = pltpu.SemaphoreType.DMA
    scratch = [
        v(16, 1024), v(16, 1024, 256), v(16, 32, 1024), v(1024, 512), v(512, 1024), v(512, 512), v(1024, 256), v(32, 1024),
        v(256, 1024), v(256, 1024), v(1024, 1024),
        v(256, 256), v(256, 128), v(256, 1, dtype=f32), v(256, 256), v(16, 256, dtype=f32),
        v(2, 1024, 256), v(2, 1024, 256), v(2, 256, 1024), v(1024, 512), v(1024, 512), v(512, 1024),
        v(8, 64, 1024), v(8, 64, 1024), v(8, 64, 1024), v(1024, 64), v(128, 1024),
        v(16, 1024), v(64, 16, 256), v(64, 16, 256), v(64, 16, 256), v(64, 16, 256), v(16, 16, 1024), v(16, 16, 1024), v(16, 16, 1024),
        dma((18,)), dma((4, 2)), dma((2, 6)), dma((1,)), dma((2, 3)), dma((2, 3)), dma((4, 3)), dma((4, 3)),
        dma, dma((4,)), dma, dma, dma, dma, dma, dma,
    ]
    return pl.pallas_call(
        kernel,
        out_shape=[jax.ShapeDtypeStruct((S, D), bf16), jax.ShapeDtypeStruct((S, C), bf16)],
        in_specs=[s for _, s in operands],
        out_specs=[vm, vm],
        scratch_shapes=scratch,
        compiler_params=pltpu.CompilerParams(
            collective_id=0, has_side_effects=True, vmem_limit_bytes=62 * 2**20
        ),
    )(*[a for a, _ in operands])


def solution(mesh):
    both = ("ep", "tp")
    by_token, whole = P(both, None), P()
    placed = (
        by_token, P(both), P(both, None, None), P(both, None, None),
        whole, whole, whole, whole, whole, whole, whole, whole, whole, whole, whole, whole, whole,
        by_token, by_token,
        P("ep", None, "tp"), P("ep", None, "tp"), P("ep", "tp", None),
        whole, whole, whole, whole,
        P(None, both), P(None, both), P(both, None), whole,
    )
    return jax.shard_map(step, mesh=mesh, in_specs=placed, out_specs=(by_token, by_token), check_vma=False)
```

```python
import math

import jax
import jax.numpy as jnp
from jax import lax
from jax.experimental import pallas as pl
from jax.experimental.pallas import tpu as pltpu
from jax.sharding import PartitionSpec as P

f32 = jnp.float32
bf16 = jnp.bfloat16
EPS = 1e-6
NT = (((1,), (1,)), ((), ()))
NN = (((1,), (0,)), ((), ()))
TN = (((0,), (0,)), ((), ()))
MESH = pl.DeviceIdType.MESH

S, H, NOPE, ROPE, L, C, D = 16, 16, 64, 32, 1024, 256, 1024
SCALE = (NOPE + ROPE) ** -0.5
CHIPS, PLANE = 64, 16
PART = 32
SLOTS, QB = 4, 4
PIECE = SLOTS * QB


def distance(k):
    return sum(min(d, 4 - d) for d in (k // 16, k // 4 % 4, k % 4))


ORDER = sorted(range(1, CHIPS), key=lambda k: (-distance(k), k * 37 % 64)) + [0]
GROUP = sorted(((kz, ky) for kz in range(4) for ky in range(4)), key=lambda k: (-distance(k[0] * 16 + k[1] * 4 + (k[0] + 2 * k[1]) % 4), k))
GROUP.remove((0, 0))


_open = []


def mark(name):
    if _open:
        _open.pop().__exit__(None, None, None)
    if name:
        scope = jax.named_scope(name)
        scope.__enter__()
        _open.append(scope)


def dot(a, b, dims=NN):
    return lax.dot_general(a, b, dims, preferred_element_type=f32)


def iota(shape, dim):
    return lax.broadcasted_iota(jnp.int32, shape, dim)


def row_of(ref):
    blocks = ref[...].astype(f32)
    return jnp.concatenate([blocks[r : r + 1, :] for r in range(blocks.shape[0])], axis=1)


def rms(value, gain):
    inverse = lax.rsqrt(jnp.mean(value * value, axis=-1, keepdims=True) + EPS)
    return value * inverse * gain


def silu(v):
    return v / (1.0 + jnp.exp(-v))


def rope_tables(len_ref):
    half = ROPE // 2
    lane = iota((S, 128), 1) % half
    row = iota((S, 128), 0)
    pos = jnp.zeros((S, 128), jnp.int32)
    for s in range(S):
        pos = jnp.where(row == s, len_ref[s], pos)
    freq = jnp.exp(lane.astype(f32) * (-math.log(10000.0) / half))
    angle = pos.astype(f32) * freq
    return jnp.cos(angle), jnp.sin(angle)


def rotate128(value, cosine, sine):
    half = ROPE // 2
    first = (iota(value.shape, 1) % ROPE) < half
    other = jnp.where(first, -pltpu.roll(value, 128 - half, 1), pltpu.roll(value, half, 1))
    return value * cosine + other * sine


def halves(value):
    high = value.astype(bf16)
    return high, (value - high.astype(f32)).astype(bf16)


def route_tables(routes, scores, pick, weigh):
    ids = routes[...].astype(bf16)
    spread = (iota((S, QB * S), 1) % S == iota((S, QB * S), 0)).astype(bf16)
    named = dot(ids, spread)
    expert = iota((CHIPS, QB * S), 0).astype(f32)
    count = jnp.zeros((CHIPS, QB * S), f32)
    for k in range(4):
        count += jnp.where(named[k : k + 1, :] == expert, 1.0, 0.0)
    r, c = iota((QB * S, QB * S), 0), iota((QB * S, QB * S), 1)
    before = ((r < S) & (r < c % S)).astype(bf16)
    rank = dot(count.astype(bf16), before)
    at = jnp.where(count > 0.5, rank, -1.0)
    shape = (CHIPS, PIECE, QB * S)
    i, n = iota(shape, 1), iota(shape, 2)
    here = (at[:, None, :] == (i % SLOTS).astype(f32)) & (i // SLOTS == n // S)
    pick[...] = jnp.where(here, 1.0, 0.0).reshape(CHIPS * PIECE, QB * S).astype(bf16)

    norm = scores[...]
    norm = norm / jnp.sum(norm, axis=0, keepdims=True) * 2.5
    high, low = halves(norm)
    select = (iota((QB * S, S), 0) % S == iota((QB * S, S), 1)).astype(bf16)
    named_t, high_t, low_t = dot(select, ids, NT), dot(select, high, NT), dot(select, low, NT)
    expert_t = iota((QB * S, CHIPS), 1).astype(f32)
    count_t = jnp.zeros((QB * S, CHIPS), f32)
    w_high, w_low = count_t, count_t
    for k in range(4):
        hit = named_t[:, k : k + 1] == expert_t
        count_t += jnp.where(hit, 1.0, 0.0)
        w_high += jnp.where(hit, high_t[:, k : k + 1], 0.0)
        w_low += jnp.where(hit, low_t[:, k : k + 1], 0.0)
    before_t = ((c < S) & (c < r % S)).astype(bf16)
    rank_t = dot(before_t, count_t.astype(bf16))
    widen = (iota((CHIPS, CHIPS * PIECE), 1) // PIECE == iota((CHIPS, CHIPS * PIECE), 0)).astype(bf16)
    shape = (QB * S, CHIPS * PIECE)
    m = iota(shape, 1)
    here = (dot(rank_t.astype(bf16), widen) == (m % SLOTS).astype(f32)) & (
        (m // SLOTS) % QB == iota(shape, 0) // S
    )
    weigh[0 : QB * S, :] = jnp.where(here, dot(w_high.astype(bf16), widen), 0.0).astype(bf16)
    weigh[QB * S : 2 * QB * S, :] = jnp.where(here, dot(w_low.astype(bf16), widen), 0.0).astype(bf16)


def kernel(
    len_ref, tok_h, lat_h, rope_h, ag, wdq_h, qg, wqn_h, wqr_h, wdkv_h, kvg, wkr_h, wuk_h, wuv_h, wo_h, pg, mg,
    routes, scores, eg_h, eu_h, ed_h, sg_h, su_h, sd_h, dvec, dg_h, du_h, dd_h, og,
    out_o, lat_o,
    tok, lat, rope, wdq, wqn, wqr, wdkv, wkr, wuk, wuv, wo, ql, qr, own_s, mixed, nlat,
    eg, eu, ed, sg, su, sd, dg, du, dd, pick, weigh,
    moe, send, recv, back, home, rows, parts, sums,
    sems, lsem, esem, zsem_s, zsem_r, fsem_s, fsem_r, asem_s, asem_r, bsem_s, bsem_r, gsem_s, gsem_r, psem_s, psem_r,
):
    mark('start')
    ep = lax.axis_index("ep")
    tp = lax.axis_index("tp")
    z, y, x = ep // 16, lax.rem(ep // 4, 4), lax.rem(ep, 4)
    zs = [lax.rem(z + i, 4) for i in range(4)]
    ys = [lax.rem(y + i, 4) for i in range(4)]
    xs = [lax.rem(x + i, 4) for i in range(4)]
    z16, y4 = [16 * v for v in zs], [4 * v for v in ys]
    zy = z16[0] + y4[0]
    place = 4 * z + y

    def chip_of(k):
        return z16[k // 16] + y4[k // 4 % 4] + xs[k % 4]

    def chip_back(k):
        return z16[-(k // 16) % 4] + y4[-(k // 4 % 4) % 4] + xs[-(k % 4) % 4]

    def member(kz, ky):
        return z16[kz] + y4[ky] + xs[(kz + 2 * ky) % 4], 4 * zs[kz] + ys[ky]

    def remote(src, dst, s_sem, r_sem, chip, core):
        return pltpu.make_async_remote_copy(
            src_ref=src, dst_ref=dst, send_sem=s_sem, recv_sem=r_sem, device_id=(chip, core), device_id_type=MESH
        )

    early = [(tok_h, tok), (wdq_h, wdq), (wdkv_h, wdkv), (wkr_h, wkr), (wqn_h, wqn), (wqr_h, wqr), (wuk_h, wuk)]
    late = [(wuv_h, wuv), (wo_h, wo), (eg_h, eg.at[0:1]), (eu_h, eu.at[0:1]), (ed_h, ed.at[0:1]),
            (sg_h, sg), (su_h, su), (sd_h, sd), (dg_h, dg.at[0]), (du_h, du.at[0]), (dd_h, dd.at[0])]
    early = [pltpu.make_async_copy(a, b, sems.at[i]) for i, (a, b) in enumerate(early)]
    late = [pltpu.make_async_copy(a, b, sems.at[7 + i]) for i, (a, b) in enumerate(late)]

    def lat_cp(g):
        return (
            pltpu.make_async_copy(lat_h.at[pl.ds(4 * g, 4)], lat.at[pl.ds(4 * g, 4)], lsem.at[g, 0]),
            pltpu.make_async_copy(rope_h.at[pl.ds(4 * g, 4)], rope.at[pl.ds(4 * g, 4)], lsem.at[g, 1]),
        )

    for c in early:
        c.start()
    for g in range(4):
        for c in lat_cp(g):
            c.start()
    for c in late:
        c.start()

    mark('greet')
    barrier = pltpu.get_barrier_semaphore()

    for k in ORDER[:-1]:
        pl.semaphore_signal(barrier, inc=1, device_id=(chip_of(k), tp), device_id_type=MESH)
    pl.semaphore_signal(barrier, inc=1, device_id=(ep, 1 - tp), device_id_type=MESH)

    mark('tables')
    route_tables(routes, scores, pick, weigh)
    mark('query')

    cosine, sine = rope_tables(len_ref)
    early[0].wait()
    tokens = tok[...].astype(f32)
    normed = rms(tokens, row_of(ag)).astype(bf16)
    early[1].wait()
    qn = rms(dot(normed, wdq[...]), row_of(qg)).astype(bf16)
    early[2].wait()
    nl = rms(dot(normed, wdkv[...]), row_of(kvg)).astype(bf16)
    nlat[...] = nl.astype(f32)
    lat_o[...] = nl
    early[3].wait()
    kr = dot(normed, jnp.concatenate([wkr[...]] * 4, axis=0), NT)
    kr = rotate128(kr, cosine, sine).astype(bf16)
    early[4].wait()
    qnope = dot(qn, wqn[...]).astype(bf16).astype(f32)
    head = iota((H, D), 1) // NOPE == iota((H, D), 0)
    qm = jnp.where(head[None], qnope[:, None, :], 0.0).reshape(S * H, D).astype(bf16)
    early[5].wait()
    qraw = dot(qn, wqr[...])
    qrot = jnp.concatenate(
        [rotate128(qraw[:, 128 * i : 128 * i + 128], cosine, sine) for i in range(4)], axis=1
    )
    qrot = qrot.astype(bf16).astype(f32)
    headr = iota((H, H * ROPE), 1) // ROPE == iota((H, H * ROPE), 0)
    qrm = jnp.where(headr[None], qrot[:, None, :], 0.0).reshape(S * H, H * ROPE).astype(bf16)
    fold = (iota((H * ROPE, 128), 0) % ROPE == iota((H * ROPE, 128), 1)).astype(bf16)
    qrf = dot(qrm, fold)
    qr[...] = qrf.astype(bf16)
    early[6].wait()
    qlat = dot(qm, wuk[...], NT).astype(bf16)
    ql[...] = qlat
    own = jnp.sum(qlat.astype(f32).reshape(S, H, C) * nl.astype(f32)[:, None, :], axis=-1, keepdims=True)
    own += jnp.sum(qrf.reshape(S, H, 128) * kr.astype(f32)[:, None, :], axis=-1, keepdims=True)
    own_s[...] = own.reshape(S * H, 1) * SCALE

    mark('barrier')
    pl.semaphore_wait(barrier, CHIPS)
    mark('weights_out')
    to_core = [
        remote(eg_h, eg.at[1:2], esem.at[0, 0], esem.at[1, 0], ep, 1 - tp),
        remote(eu_h, eu.at[1:2], esem.at[0, 1], esem.at[1, 1], ep, 1 - tp),
        remote(ed_h, ed.at[1:2], esem.at[0, 2], esem.at[1, 2], ep, 1 - tp),
        remote(dg_h, dg.at[4], esem.at[0, 3], esem.at[1, 3], ep, 1 - tp),
        remote(du_h, du.at[4], esem.at[0, 4], esem.at[1, 4], ep, 1 - tp),
        remote(dd_h, dd.at[4], esem.at[0, 5], esem.at[1, 5], ep, 1 - tp),
    ]
    step = 3 - 2 * tp
    sides = [zy + lax.rem(x + step, 4), z16[0] + 4 * lax.rem(y + step, 4) + x, 16 * lax.rem(z + step, 4) + y4[0] + x]
    to_chips = []
    for j in range(3):
        for i, (h, buf) in enumerate([(dg_h, dg), (du_h, du), (dd_h, dd)]):
            to_chips.append(remote(h, buf.at[1 + j], zsem_s.at[j, i], zsem_r.at[j, i], sides[j], tp))
    for c in to_chips + to_core:
        c.start()

    lane = iota((H, L), 1)

    def group(g, _):
        for c in lat_cp(g):
            c.wait()
        base = pl.multiple_of(g * 4 * H, 4 * H)
        rows4 = pl.ds(base, 4 * H)
        sc = jnp.concatenate(
            [
                dot(ql[pl.ds(base + i * H, H)], lat[g * 4 + i], NT)
                + dot(qr[pl.ds(base + i * H, H), :][:, :ROPE], rope[g * 4 + i])
                for i in range(4)
            ],
            axis=0,
        )
        sc = sc * SCALE
        valid = jnp.concatenate([lane < len_ref[g * 4 + i] for i in range(4)], axis=0)
        ow = own_s[rows4]
        top = jnp.maximum(jnp.max(jnp.where(valid, sc, -1e30), axis=-1, keepdims=True), ow)
        w = jnp.where(valid, jnp.exp(sc - top), 0.0)
        ow = jnp.exp(ow - top)
        inv = 1.0 / (jnp.sum(w, axis=-1, keepdims=True) + ow)
        pb = (w * inv).astype(bf16)
        ob = (ow * inv).astype(bf16).astype(f32)
        for i in range(4):
            m = dot(pb[i * H : i * H + H], lat[g * 4 + i]) + ob[i * H : i * H + H] * nlat[pl.ds(g * 4 + i, 1)]
            mixed[pl.ds(base + i * H, H)] = m.astype(bf16)
        return 0

    mark('cache')
    lax.fori_loop(0, 4, group, 0)
    mark('attn_out')
    late[0].wait()
    full = dot(mixed[...], wuv[...]).reshape(S, H, D)
    ho = jnp.sum(jnp.where(head[None], full, 0.0), axis=1).astype(bf16)
    late[1].wait()
    first = (tokens + rms(dot(ho, wo[...]), row_of(pg))).astype(bf16)
    moe_in = rms(first.astype(f32), row_of(mg)).astype(bf16)
    moe[...] = moe_in

    mark('pack')
    blocks = jnp.concatenate([moe_in[:, 256 * q : 256 * q + 256] for q in range(QB)], axis=0)
    send[...] = dot(pick[...], blocks).astype(bf16).reshape(CHIPS, PIECE, 256)
    recv[CHIPS - 1] = send[ep]
    rows[place] = moe_in
    mark('dispatch')
    for i, k in enumerate(ORDER[:-1]):
        chip = chip_of(k)
        remote(send.at[chip], recv.at[i], asem_s, asem_r.at[i // PART], chip, tp).start()
    for k in GROUP:
        remote(moe, rows.at[place], gsem_s, gsem_r, member(*k)[0], tp).start()

    mark('onward')
    crossing = []
    for j in range(3):
        for i, buf in enumerate([dg, du, dd]):
            to_chips[3 * j + i].wait_recv()
            crossing.append(remote(buf.at[1 + j], buf.at[5 + j], fsem_s.at[j, i], fsem_r.at[j, i], ep, 1 - tp))
    for c in crossing:
        c.start()

    mark('shared')
    for c in late[5:8]:
        c.wait()
    shared_act = (silu(dot(moe_in, sg[...])) * dot(moe_in, su[...])).astype(bf16)
    mixture = dot(shared_act, sd[...])

    mark('expert_w')
    for c in late[2:5]:
        c.wait()
    for c in to_core[0:3]:
        c.wait_recv()
    m, n = iota((256, 256), 0), iota((256, 256), 1)
    sort = ((m // 64 == (n // SLOTS) % QB) & ((m % 64) // SLOTS == n // PIECE) & (m % SLOTS == n % SLOTS))
    sort = jnp.where(sort, 1.0, 0.0).astype(bf16)
    for g in range(CHIPS // PART):
        mark('expert_wait')
        lo, others = g * PART, PART - (g == CHIPS // PART - 1)
        pltpu.make_async_copy(recv.at[0:others], recv.at[0:others], asem_r.at[g]).wait()
        mark('expert')
        rows_in = []
        for h in range(lo, lo + PART, PLANE):
            got = dot(sort, recv[h : h + PLANE].reshape(PLANE * PIECE, 256)).astype(bf16)
            rows_in.append(jnp.concatenate([got[64 * q : 64 * q + 64] for q in range(QB)], axis=1))
        rows_in = jnp.concatenate(rows_in, axis=0)
        total = jnp.zeros((PART * SLOTS, D), f32)
        for part in range(2):
            act = (silu(dot(rows_in, eg[part])) * dot(rows_in, eu[part])).astype(bf16)
            total += dot(act, ed[part]).astype(bf16).astype(f32)
        total = total.astype(bf16)
        for j, h in enumerate(range(lo, lo + PART, PLANE)):
            some = total[64 * j : 64 * j + 64]
            some = jnp.concatenate([some[:, 256 * q : 256 * q + 256] for q in range(QB)], axis=0)
            back[h : h + PLANE] = dot(sort, some, TN).astype(bf16).reshape(PLANE, PIECE, 256)
        mark('give')
        for i in range(lo, lo + others):
            remote(back.at[i], home.at[ep], bsem_s, bsem_r, chip_back(ORDER[i]), tp).start()
    home[ep] = back[CHIPS - 1]

    mark('dense_w')
    for c in late[8:11]:
        c.wait()
    for c in to_core[3:6] + crossing:
        c.wait_recv()
    pltpu.make_async_copy(rows.at[0:15], rows.at[0:15], gsem_r).wait()
    mark('dense')
    all_rows = rows[...].reshape(PLANE * S, D)
    gate_h = dot(all_rows, dg[...].reshape(512, D), NT)
    up_h = dot(all_rows, du[...].reshape(512, D), NT)
    act = (silu(gate_h) * up_h).astype(bf16)
    parts[...] = dot(act, dd[...].reshape(512, D)).astype(bf16).reshape(PLANE, S, D)
    sums[place] = parts[place]
    mark('share')
    for k in GROUP:
        chip, its = member(*k)
        remote(parts.at[its], sums.at[place], psem_s, psem_r, chip, tp).start()

    gate = jnp.sum(moe_in.astype(f32) * row_of(dvec), axis=-1, keepdims=True)
    gate = 1.0 / (1.0 + jnp.exp(-gate))

    mark('home_wait')
    pltpu.make_async_copy(home.at[0:63], home.at[0:63], bsem_r).wait()
    mark('routed')
    routed = dot(weigh[...], home[...].reshape(CHIPS * PIECE, 256))
    routed = routed[0:64] + routed[64:128]
    mixture += jnp.concatenate([routed[S * q : S * q + S] for q in range(QB)], axis=1)

    mark('sums_wait')
    pltpu.make_async_copy(sums.at[0:15], sums.at[0:15], psem_r).wait()
    mark('final')
    dense = jnp.zeros((S, D), f32)
    for p in range(PLANE):
        dense += sums[p].astype(f32)
    mixture += gate * dense
    out_o[...] = (first.astype(f32) + rms(mixture, row_of(og))).astype(bf16)

    mark('drain')
    for c in to_chips + to_core + crossing:
        c.wait_send()
    pltpu.make_async_copy(send.at[0:63], send.at[0:63], asem_s).wait()
    pltpu.make_async_copy(back.at[0:63], back.at[0:63], bsem_s).wait()
    pltpu.make_async_copy(rows.at[0:15], rows.at[0:15], gsem_s).wait()
    pltpu.make_async_copy(parts.at[0:15], parts.at[0:15], psem_s).wait()
    mark(None)


def put_out(a, b, a_o, b_o, sems):
    copies = [pltpu.make_async_copy(a, a_o, sems.at[0]), pltpu.make_async_copy(b, b_o, sems.at[1])]
    for c in copies:
        c.start()
    for c in copies:
        c.wait()


def step(
    tokens, lengths, latent, rope, ag, wdq, qg, wqn, wqr, wdkv, kvg, wkr, wuk, wuv, wo, pg, mg,
    routes, scores, eg, eu, ed, sg, su, sd, dvec, dg, du, dd, og,
):
    anyspec = pl.BlockSpec(memory_space=pl.ANY)
    vm = pl.BlockSpec(memory_space=pltpu.VMEM)
    smem = pl.BlockSpec(memory_space=pltpu.SMEM)

    def tile(v):
        return v.reshape(v.shape[0] // 128, 128)

    operands = [
        (lengths, smem), (tokens, anyspec), (latent, anyspec), (rope, anyspec), (tile(ag), vm), (wdq, anyspec), (tile(qg), vm),
        (wqn, anyspec), (wqr, anyspec), (wdkv, anyspec), (tile(kvg), vm), (wkr.T, anyspec), (wuk, anyspec), (wuv, anyspec),
        (wo, anyspec), (tile(pg), vm), (tile(mg), vm), (routes.T, vm), (scores.T, vm), (eg, anyspec), (eu, anyspec),
        (ed, anyspec), (sg, anyspec), (su, anyspec), (sd, anyspec), (tile(dvec), vm), (dg.T, anyspec), (du.T, anyspec),
        (dd, anyspec), (tile(og), vm),
    ]

    def v(*shape, dtype=bf16):
        return pltpu.VMEM(shape, dtype)

    dma = pltpu.SemaphoreType.DMA
    scratch = [
        v(16, 1024), v(16, 1024, 256), v(16, 32, 1024), v(1024, 512), v(512, 1024), v(512, 512), v(1024, 256), v(32, 1024),
        v(256, 1024), v(256, 1024), v(1024, 1024),
        v(256, 256), v(256, 128), v(256, 1, dtype=f32), v(256, 256), v(16, 256, dtype=f32),
        v(2, 1024, 256), v(2, 1024, 256), v(2, 256, 1024), v(1024, 512), v(1024, 512), v(512, 1024),
        v(8, 64, 1024), v(8, 64, 1024), v(8, 64, 1024), v(1024, 64), v(128, 1024),
        v(16, 1024), v(64, 16, 256), v(64, 16, 256), v(64, 16, 256), v(64, 16, 256), v(16, 16, 1024), v(16, 16, 1024), v(16, 16, 1024),
        dma((18,)), dma((4, 2)), dma((2, 6)), dma((3, 3)), dma((3, 3)), dma((3, 3)), dma((3, 3)),
        dma, dma((CHIPS // PART,)), dma, dma, dma, dma, dma, dma,
    ]
    results = pl.pallas_call(
        kernel,
        out_shape=[pltpu.VMEM((S, D), bf16), pltpu.VMEM((S, C), bf16)],
        in_specs=[s for _, s in operands],
        out_specs=[vm, vm],
        scratch_shapes=scratch,
        compiler_params=pltpu.CompilerParams(
            collective_id=0, has_side_effects=True, vmem_limit_bytes=62 * 2**20
        ),
    )(*[a for a, _ in operands])
    return pl.pallas_call(
        put_out,
        out_shape=[jax.ShapeDtypeStruct((S, D), bf16), jax.ShapeDtypeStruct((S, C), bf16)],
        in_specs=[vm, vm],
        out_specs=[anyspec, anyspec],
        scratch_shapes=[dma((2,))],
    )(*[pltpu.with_memory_space_constraint(r, pltpu.VMEM) for r in results])


def solution(mesh):
    both = ("ep", "tp")
    by_token, whole = P(both, None), P()
    placed = (
        by_token, P(both), P(both, None, None), P(both, None, None),
        whole, whole, whole, whole, whole, whole, whole, whole, whole, whole, whole, whole, whole,
        by_token, by_token,
        P("ep", None, "tp"), P("ep", None, "tp"), P("ep", "tp", None),
        whole, whole, whole, whole,
        P(None, both), P(None, both), P(both, None), whole,
    )
    return jax.shard_map(step, mesh=mesh, in_specs=placed, out_specs=(by_token, by_token), check_vma=False)
```
